32 devices in a mesh: kv: 4 (over y, x), tp: 8 (over z, core).
Axes of the slice: x: 2, y: 2, z: 4, core: 2. Of those that a mesh axis runs over, the one named last changes fastest.
Arguments:
- residual: bfloat16 [128, 4096], P(None, ('kv', 'tp')), may hold values from -20 to 20
- mixer_gain: float32 [4096], P('kv'), may hold values from 0.1 to 1.9
- w_query: bfloat16 [4096, 4096], P('kv', 'tp'), may hold values from -0.09375 to 0.09375
- w_forget: bfloat16 [4096, 4096], P('kv', 'tp'), may hold values from -0.09375 to 0.09375
- w_input: bfloat16 [4096, 4096], P('kv', 'tp'), may hold values from -0.09375 to 0.09375
- w_outgate: bfloat16 [4096, 4096], P('kv', 'tp'), may hold values from -0.09375 to 0.09375
- lower_bound: float32 [4096], P('tp'), may hold values from 0.3 to 0.97
- state: float32 [128, 32, 128, 128], P('kv', 'tp'), may hold values from -6 to 6
- head_gain: float32 [128], replicated, may hold values from 0.1 to 1.9
- w_mix_out: bfloat16 [4096, 4096], P('tp', 'kv'), may hold values from -0.09375 to 0.09375
- ffn_gain: float32 [4096], P('kv'), may hold values from 0.1 to 1.9
- w_gate: bfloat16 [4096, 10752], P('kv', 'tp'), may hold values from -0.09375 to 0.09375
- w_up: bfloat16 [4096, 10752], P('kv', 'tp'), may hold values from -0.09375 to 0.09375
- w_down: bfloat16 [10752, 4096], P('tp', 'kv'), may hold values from -0.0625 to 0.0625
Outputs:
- layer_out: bfloat16 [128, 4096], P(None, ('kv', 'tp'))
- new_state: float32 [128, 32, 128, 128], P('kv', 'tp')
The draws below stay inside these ranges and needn't reach their ends.
All inputs are finite; a program needn't handle non-finite values.
Results may differ from the reference program's by a relative error of at most 0.015.
Values may be sent and summed in bfloat16 or wider, within the bound.
No kernel may reach another device: no remote copies, remote signals or barrier semaphores. Data moves between devices by JAX's collectives and lax.ppermute only.
A program may use at most 64 MiB of HBM per device.

```python
import jax
import jax.numpy as jnp
from jax import lax

D = 4096
HEADS = 32
DK = 128
DV = 128
FF = 10752
SEQS = 128
HID = 4096
VID = 4096
N_KV = 4
N_TP = 8


def draw_residual(key, part):
    first = jax.random.fold_in(jax.random.fold_in(key, 11), 0)
    column = jnp.arange(D)
    kv_index = (column // (D // N_KV)).astype(jnp.float32)
    tp_index = (column // (D // (N_KV * N_TP)) % N_TP).astype(jnp.float32)
    col_scale = 0.4 * 3.0 ** (kv_index / max(N_KV - 1, 1)) * 3.0 ** (tp_index / max(N_TP - 1, 1))
    values = jnp.clip(jax.random.normal(first, (SEQS, D), jnp.float32), -4.0, 4.0)
    return jnp.clip(values * col_scale, -20.0, 20.0).astype(jnp.bfloat16)


def block_scale(stream_key, extent, pieces, smallest, high):
    gain = 1.0
    for position, shards_of in pieces:
        heights = jax.random.uniform(jax.random.fold_in(jax.random.fold_in(stream_key, 6), position), (shards_of,), jnp.float32, smallest / len(pieces), high / len(pieces))
        gain = gain * jnp.repeat(jnp.exp(heights), extent[position] // shards_of).reshape((-1,) + (1,) * (len(extent) - 1 - position))
    return gain


def scatter_about(stream_key, dims, scale, most, cuts=(), held_as=jnp.bfloat16):
    drawn = scale * jax.random.normal(stream_key, dims, jnp.float32)
    if cuts:
        drawn = drawn * block_scale(stream_key, dims, cuts, -0.22, 0.18)
    return jnp.clip(drawn, -most, most).astype(held_as)


def setup_inputs(seed: int = 0) -> dict:
    key_of = jax.random.split(jax.random.key(seed), 15)
    return {
        "residual": draw_residual(jax.random.fold_in(key_of[14], 71), 0),
        "mixer_gain": jnp.clip(1.0 + 0.18 * jax.random.normal(key_of[1], (D,), jnp.float32), 0.1, 1.9),
        "w_query": scatter_about(key_of[2], (D, HID), D ** -0.5, 0.09375, ((0, 4), (1, 8))),
        "w_forget": scatter_about(key_of[3], (D, HID), D ** -0.5, 0.09375, ((0, 4), (1, 8))),
        "w_input": scatter_about(key_of[4], (D, VID), D ** -0.5, 0.09375, ((0, 4), (1, 8))),
        "w_outgate": scatter_about(key_of[5], (D, VID), D ** -0.5, 0.09375, ((0, 4), (1, 8))),
        "lower_bound": jnp.clip(0.3 + 0.67 * jax.random.uniform(key_of[6], (HID,), jnp.float32) ** block_scale(key_of[6], (HID,), ((0, 8),), -0.2, 0.2), 0.3, 0.97),
        "state": scatter_about(key_of[7], (SEQS, HEADS, DK, DV), 1.0, 6.0, ((0, 4), (1, 8)), jnp.float32),
        "head_gain": jnp.clip(1.0 + 0.18 * jax.random.normal(key_of[8], (DV,), jnp.float32), 0.1, 1.9),
        "w_mix_out": scatter_about(key_of[9], (VID, D), VID ** -0.5, 0.09375, ((0, 8), (1, 4))),
        "ffn_gain": jnp.clip(1.0 + 0.18 * jax.random.normal(key_of[10], (D,), jnp.float32), 0.1, 1.9),
        "w_gate": scatter_about(key_of[11], (D, FF), D ** -0.5, 0.09375, ((0, 4), (1, 8))),
        "w_up": scatter_about(key_of[12], (D, FF), D ** -0.5, 0.09375, ((0, 4), (1, 8))),
        "w_down": scatter_about(key_of[13], (FF, D), FF ** -0.5, 0.0625, ((0, 8), (1, 4))),
    }


EPS = 1e-06

def reference(residual, mixer_gain, w_query, w_forget, w_input, w_outgate, lower_bound, state, head_gain, w_mix_out, ffn_gain, w_gate, w_up, w_down):
    seqs = residual.shape[0]
    xf = residual.astype(jnp.float32)
    inv_a = lax.rsqrt(lax.optimization_barrier(jnp.mean(xf * xf, axis=1, keepdims=True)) + EPS)
    scaled_a = (xf * mixer_gain).astype(jnp.bfloat16)
    query_raw = inv_a * jnp.dot(scaled_a, w_query, preferred_element_type=jnp.float32)
    forget_raw = inv_a * jnp.dot(scaled_a, w_forget, preferred_element_type=jnp.float32)
    value_raw = inv_a * jnp.dot(scaled_a, w_input, preferred_element_type=jnp.float32)
    outgate_raw = inv_a * jnp.dot(scaled_a, w_outgate, preferred_element_type=jnp.float32)
    bound = lower_bound.reshape(HEADS, DK)
    forget_raw = forget_raw.reshape(seqs, HEADS, DK)
    forget = bound + (1.0 - bound) * jax.nn.sigmoid(forget_raw)
    keyvec = (1.0 - bound) * jax.nn.sigmoid(-forget_raw)
    query = jax.nn.silu(query_raw.reshape(seqs, HEADS, DK))
    values = value_raw.reshape(seqs, HEADS, DV)
    new_state = forget[..., None] * state + keyvec[..., None] * values[:, :, None, :]
    head_out = jnp.einsum('shc,shce->she', query, new_state, precision=lax.Precision.HIGHEST)
    inv_h = lax.rsqrt(lax.optimization_barrier(jnp.mean(head_out * head_out, axis=2, keepdims=True)) + EPS)
    normed = head_out * inv_h * head_gain * jax.nn.silu(outgate_raw.reshape(seqs, HEADS, DV))
    normed = normed.reshape(seqs, HEADS * DV).astype(jnp.bfloat16)
    after_mix = (xf + jnp.dot(normed, w_mix_out, preferred_element_type=jnp.float32)).astype(jnp.bfloat16)
    af = after_mix.astype(jnp.float32)
    inv_b = lax.rsqrt(lax.optimization_barrier(jnp.mean(af * af, axis=1, keepdims=True)) + EPS)
    scaled_b = (af * ffn_gain).astype(jnp.bfloat16)
    gate = inv_b * jnp.dot(scaled_b, w_gate, preferred_element_type=jnp.float32)
    upper = inv_b * jnp.dot(scaled_b, w_up, preferred_element_type=jnp.float32)
    hidden = (jax.nn.silu(gate) * upper).astype(jnp.bfloat16)
    layer_out = (af + jnp.dot(hidden, w_down, preferred_element_type=jnp.float32)).astype(jnp.bfloat16)
    return (layer_out, new_state)
```

```python
import functools

import jax
import jax.numpy as jnp
from jax import lax
from jax.experimental import pallas as pl
from jax.experimental.pallas import tpu as pltpu
from jax.sharding import PartitionSpec as P

EPS = 1e-06
LANES = 128
PAIR = 2
BF16 = jnp.bfloat16
F32 = jnp.float32


def exchange(value, axis, size, mask):
    return lax.ppermute(value, axis, [(i, i ^ mask) for i in range(size)])


def call(kernel, out_shape, scratch=(), **kwargs):
    return pl.pallas_call(kernel, out_shape=out_shape, scratch_shapes=list(scratch), **kwargs)


def tail_pieces(total, first_lane):
    lane = lax.broadcasted_iota(jnp.int32, (total.shape[0], LANES), 1) - first_lane
    high = total.astype(BF16).astype(F32)
    middle = (total - high).astype(BF16).astype(F32)
    low = total - high - middle
    zero = jnp.zeros((), F32)
    return jnp.where(
        lane == 0, high, jnp.where(lane == 1, middle, jnp.where(lane == 2, low, zero))
    )


def product(left, right):
    return jnp.dot(left, right, preferred_element_type=F32)


def gather_scaled(near_ref, far_ref, gain_ref, blocks_ref, count):
    own = lax.axis_index("tp")
    squares = None
    for k in range(count):
        for ref, source in ((near_ref, own ^ (PAIR * k)), (far_ref, own ^ (PAIR * k + 1))):
            block = ref[k].astype(F32)
            squares = block * block if squares is None else squares + block * block
            blocks_ref[source] = (block * gain_ref[source]).astype(BF16)
    rows = jnp.concatenate([blocks_ref[j] for j in range(PAIR * count)], axis=1)
    return rows, jnp.sum(squares, axis=1, keepdims=True)


def spread(parts_ref, own_ref, send_refs):
    own = lax.axis_index("kv")
    own_ref[...] = parts_ref[own]
    for mask, ref in enumerate(send_refs, 1):
        ref[...] = parts_ref[own ^ mask].astype(BF16)


def project_kernel(near_ref, far_ref, gain_ref, *refs, count, n_weights, offsets, tail, local):
    weights, outs = refs[:n_weights], refs[n_weights:-2]
    blocks_ref, parts_ref = refs[-2:]
    rows, squares = gather_scaled(near_ref, far_ref, gain_ref, blocks_ref, count)
    groups = parts_ref.shape[0]
    start = tail // LANES * LANES
    pieces = tail_pieces(squares, tail - start)

    def put(value, at):
        for d in range(groups):
            parts_ref[d, :, at : at + value.shape[1]] = value[d * local : (d + 1) * local]

    zero = jnp.zeros((rows.shape[0], LANES), F32)
    put(zero, parts_ref.shape[2] - LANES)
    put(pieces, start)
    for weight, at in zip(weights, offsets):
        put(product(rows, weight[...]), at)
    spread(parts_ref, outs[0], outs[1:])


def project(near, far, gain, weights, offsets, tail, width, n_kv):
    count, seqs, block = near.shape
    local = seqs // n_kv
    kernel = functools.partial(
        project_kernel,
        count=count,
        n_weights=len(weights),
        offsets=offsets,
        tail=tail,
        local=local,
    )
    outs = [jax.ShapeDtypeStruct((local, width), F32)]
    outs += [jax.ShapeDtypeStruct((local, width), BF16)] * (n_kv - 1)
    scratch = [
        pltpu.VMEM((PAIR * count, seqs, block), BF16),
        pltpu.VMEM((n_kv, local, width), F32),
    ]
    gains = gain.reshape(PAIR * count, 1, block)
    return call(kernel, outs, scratch)(near, far, gains, *weights)


def recur_kernel(*refs, n_parts, model, heads, keys, values):
    parts = refs[:n_parts]
    bound_ref, gain_ref, state_ref, new_ref, normed_ref = refs[n_parts:]
    raw = parts[0][...]
    for ref in parts[1:]:
        raw = raw + ref[...].astype(F32)
    total = jnp.sum(raw[:, -LANES:], axis=1, keepdims=True)
    raw = raw * lax.rsqrt(total / model + EPS)
    local = raw.shape[0]
    hid = heads * keys
    bound = bound_ref[...]
    query = jax.nn.silu(raw[:, :hid])
    forget_raw = raw[:, hid : 2 * hid]
    forget = bound + (1.0 - bound) * jax.nn.sigmoid(forget_raw)
    keyvec = (1.0 - bound) * jax.nn.sigmoid(-forget_raw)
    value = raw[:, 2 * hid : 2 * hid + heads * values]
    out_gate = jax.nn.silu(raw[:, 2 * hid + heads * values : 2 * (hid + heads * values)])
    for h in range(heads):
        span = slice(h * keys, (h + 1) * keys)
        columns = jnp.concatenate([query[:, span], forget[:, span], keyvec[:, span]], axis=0).T
        spread_values = slice(h * values, (h + 1) * values)
        rows = []
        for s in range(local):
            q = columns[:, s : s + 1]
            f = columns[:, local + s : local + s + 1]
            k = columns[:, 2 * local + s : 2 * local + s + 1]
            new = f * state_ref[s, h] + k * value[s : s + 1, spread_values]
            new_ref[s, h] = new
            rows.append(jnp.sum(q * new, axis=0, keepdims=True))
        head_out = jnp.concatenate(rows, axis=0)
        scale = lax.rsqrt(jnp.mean(head_out * head_out, axis=1, keepdims=True) + EPS)
        normed = head_out * scale * gain_ref[...] * out_gate[:, spread_values]
        normed_ref[:, spread_values] = normed.astype(BF16)


def recur(parts, lower_bound, head_gain, state, model):
    local, heads, keys, values = state.shape
    step = 8
    width = parts[0].shape[1]
    kernel = functools.partial(
        recur_kernel, n_parts=len(parts), model=model, heads=heads, keys=keys, values=values
    )
    row = lambda i: (i, 0)
    fixed = lambda i: (0, 0)
    cube = pl.BlockSpec((step, heads, keys, values), lambda i: (i, 0, 0, 0))
    return pl.pallas_call(
        kernel,
        grid=(local // step,),
        in_specs=[pl.BlockSpec((step, width), row)] * len(parts)
        + [
            pl.BlockSpec((1, heads * keys), fixed),
            pl.BlockSpec((1, values), fixed),
            cube,
        ],
        out_specs=[cube, pl.BlockSpec((step, heads * values), row)],
        out_shape=[
            jax.ShapeDtypeStruct(state.shape, F32),
            jax.ShapeDtypeStruct((local, heads * values), BF16),
        ],
    )(*parts, lower_bound.reshape(1, heads * keys), head_gain.reshape(1, values), state)


def mix_kernel(*refs, n_parts, local, count):
    parts = refs[:n_parts]
    weight_ref, keep_ref, send_ref, rows_ref, terms_ref = refs[n_parts:]
    own = lax.axis_index("kv")
    core = lax.axis_index("tp") % PAIR
    depth = weight_ref.shape[0]
    for mask, ref in enumerate(parts):
        rows_ref[own ^ mask] = ref[...]
    rows = jnp.concatenate([rows_ref[d] for d in range(n_parts)], axis=0)
    terms = product(rows[:, :depth], weight_ref[...])
    block = terms.shape[1] // (PAIR * count)
    for j in range(PAIR * count):
        terms_ref[j] = terms[:, j * block : (j + 1) * block]
    for z in range(count):
        keep_ref[z] = terms_ref[PAIR * z + core]
        send_ref[z] = terms_ref[PAIR * z + 1 - core].astype(BF16)


def mix(parts, weight, count):
    local, width = parts[0].shape
    n_kv = len(parts)
    seqs = local * n_kv
    block = weight.shape[1] // (PAIR * count)
    kernel = functools.partial(mix_kernel, n_parts=n_kv, local=local, count=count)
    outs = [
        jax.ShapeDtypeStruct((count, seqs, block), F32),
        jax.ShapeDtypeStruct((count, seqs, block), BF16),
    ]
    scratch = [
        pltpu.VMEM((n_kv, local, width), BF16),
        pltpu.VMEM((PAIR * count, seqs, block), F32),
    ]
    return call(kernel, outs, scratch)(*parts, weight)


def fold_kernel(keep_ref, far_ref, own_ref, *send_refs):
    z = lax.axis_index("tp") // PAIR
    own_ref[...] = keep_ref[z] + far_ref[z].astype(F32)
    for mask, ref in enumerate(send_refs, 1):
        ref[...] = (keep_ref[z ^ mask] + far_ref[z ^ mask].astype(F32)).astype(BF16)


def finish_kernel(base_ref, *refs):
    total = base_ref[...].astype(F32)
    for ref in refs[:-1]:
        total = total + ref[...].astype(F32)
    refs[-1][...] = total.astype(BF16)


def reduce_tp(keep, send, base, n_tp):
    count, seqs, block = keep.shape
    far = exchange(send, "tp", n_tp, 1)
    outs = [jax.ShapeDtypeStruct((seqs, block), F32)]
    outs += [jax.ShapeDtypeStruct((seqs, block), BF16)] * (count - 1)
    own, *sends = call(fold_kernel, outs)(keep, far)
    got = [exchange(v, "tp", n_tp, PAIR * k) for k, v in enumerate(sends, 1)]
    return call(finish_kernel, jax.ShapeDtypeStruct((seqs, block), BF16))(base, own, *got)


def gather_tp(block, n_tp):
    count = n_tp // PAIR
    near = jnp.stack([block] + [exchange(block, "tp", n_tp, PAIR * k) for k in range(1, count)])
    return near, exchange(near, "tp", n_tp, 1)


def hidden_kernel(*refs, model, tail):
    raw = refs[0][...]
    for ref in refs[1:-1]:
        raw = raw + ref[...].astype(F32)
    half = raw.shape[1] // 2
    start = tail // LANES * LANES
    lane = lax.broadcasted_iota(jnp.int32, (raw.shape[0], LANES), 1)
    pieces = jnp.where(lane >= tail - start, raw[:, start : start + LANES], 0.0)
    inverse = lax.rsqrt(jnp.sum(pieces, axis=1, keepdims=True) / model + EPS)
    gate = raw[:, :half] * inverse
    refs[-1][...] = (jax.nn.silu(gate) * (raw[:, half:] * inverse)).astype(BF16)


def fast_body(
    residual,
    mixer_gain,
    w_query,
    w_forget,
    w_input,
    w_outgate,
    lower_bound,
    state,
    head_gain,
    w_mix_out,
    ffn_gain,
    w_gate,
    w_up,
    w_down,
    *,
    n_kv,
    n_tp,
):
    count = n_tp // PAIR
    model = residual.shape[1] * n_kv * n_tp
    local = state.shape[0]
    kv_masks = range(1, n_kv)

    near, far = gather_tp(residual, n_tp)
    weights = (w_query, w_forget, w_input, w_outgate)
    offsets, at = [], 0
    for weight in weights:
        offsets.append(at)
        at += weight.shape[1]
    own, *sends = project(near, far, mixer_gain, weights, offsets, at, at + LANES, n_kv)
    parts = [own] + [exchange(v, "kv", n_kv, m) for m, v in zip(kv_masks, sends)]
    new_state, normed = recur(parts, lower_bound, head_gain, state, model)

    parts = [normed] + [exchange(normed, "kv", n_kv, m) for m in kv_masks]
    keep, send = mix(parts, w_mix_out, count)
    after_mix = reduce_tp(keep, send, residual, n_tp)

    near, far = gather_tp(after_mix, n_tp)
    units = w_gate.shape[1]
    padded = (units + 3 + LANES - 1) // LANES * LANES
    own, *sends = project(
        near, far, ffn_gain, (w_gate, w_up), (0, padded), units, 2 * padded, n_kv
    )
    parts = [own] + [exchange(v, "kv", n_kv, m) for m, v in zip(kv_masks, sends)]
    hidden = call(
        functools.partial(hidden_kernel, model=model, tail=units),
        jax.ShapeDtypeStruct((local, padded), BF16),
    )(*parts)
    parts = [hidden] + [exchange(hidden, "kv", n_kv, m) for m in kv_masks]
    keep, send = mix(parts, w_down, count)
    return reduce_tp(keep, send, after_mix, n_tp), new_state


def project_row(weight, piece):
    return jnp.dot(piece, weight, preferred_element_type=jnp.float32)


def channel_mix(rows_in, model, ffn_gain, w_gate, w_up, w_down):
    rows_float = rows_in.astype(jnp.float32)
    squares = jnp.sum(rows_float * rows_float, axis=1)
    scaled = (rows_float * ffn_gain).astype(jnp.bfloat16)
    gate = jnp.dot(scaled, w_gate, preferred_element_type=jnp.float32)
    upper = jnp.dot(scaled, w_up, preferred_element_type=jnp.float32)
    whole_total = lax.psum(squares, "kv")
    gate, upper = (
        lax.psum(gate.astype(jnp.bfloat16), "kv").astype(jnp.float32),
        lax.psum(upper.astype(jnp.bfloat16), "kv").astype(jnp.float32),
    )
    inverse = lax.rsqrt(whole_total / model + EPS)[:, None]
    hidden = (jax.nn.silu(gate * inverse) * (upper * inverse)).astype(jnp.bfloat16)
    terms = jnp.dot(hidden, w_down, preferred_element_type=jnp.float32)
    summed = lax.psum_scatter(
        terms.astype(jnp.bfloat16), "tp", scatter_dimension=1, tiled=True
    ).astype(jnp.float32)
    width = summed.shape[1]
    own = lax.dynamic_slice_in_dim(rows_float, lax.axis_index("tp") * width, width, 1)
    return (own + summed).astype(jnp.bfloat16)


def plain_body(
    residual,
    mixer_gain,
    w_query,
    w_forget,
    w_input,
    w_outgate,
    lower_bound,
    state,
    head_gain,
    w_mix_out,
    ffn_gain,
    w_gate,
    w_up,
    w_down,
    *,
    n_kv,
    n_tp,
):
    local_seqs, local_heads, DK, DV = state.shape
    model = residual.shape[1] * n_kv * n_tp
    rows = lax.all_gather(residual, "tp", axis=1, tiled=True)
    rows_float = rows.astype(jnp.float32)
    squares = jnp.sum(rows_float * rows_float, axis=1)
    scaled = (rows_float * mixer_gain).astype(jnp.bfloat16)
    part_query = jnp.dot(scaled, w_query, preferred_element_type=jnp.float32)
    part_forget = jnp.dot(scaled, w_forget, preferred_element_type=jnp.float32)
    part_value = jnp.dot(scaled, w_input, preferred_element_type=jnp.float32)
    part_gate = jnp.dot(scaled, w_outgate, preferred_element_type=jnp.float32)
    whole_total = lax.psum(squares, "kv")
    total = lax.dynamic_slice_in_dim(whole_total, lax.axis_index("kv") * local_seqs, local_seqs)
    part_query, part_forget, part_value, part_gate = (
        lax.psum_scatter(part_query, "kv", scatter_dimension=0, tiled=True),
        lax.psum_scatter(part_forget, "kv", scatter_dimension=0, tiled=True),
        lax.psum_scatter(part_value, "kv", scatter_dimension=0, tiled=True),
        lax.psum_scatter(part_gate, "kv", scatter_dimension=0, tiled=True),
    )
    inverse = lax.rsqrt(total / model + EPS)[:, None]
    bound = lower_bound.reshape(local_heads, DK)
    forget_raw = (part_forget * inverse).reshape(local_seqs, local_heads, DK)
    forget = bound + (1.0 - bound) * jax.nn.sigmoid(forget_raw)
    keyvec = (1.0 - bound) * jax.nn.sigmoid(-forget_raw)
    query = jax.nn.silu((part_query * inverse).reshape(local_seqs, local_heads, DK))
    values = (part_value * inverse).reshape(local_seqs, local_heads, DV)
    updated = forget[..., None] * state + keyvec[..., None] * values[:, :, None, :]
    head_out = jnp.einsum("shc,shce->she", query, updated, precision=lax.Precision.HIGHEST)
    inv_head = lax.rsqrt(jnp.mean(head_out * head_out, axis=2, keepdims=True) + EPS)
    out_gate = jax.nn.silu((part_gate * inverse).reshape(local_seqs, local_heads, DV))
    normed = (
        (head_out * inv_head * head_gain * out_gate)
        .reshape(local_seqs, local_heads * DV)
        .astype(jnp.bfloat16)
    )
    terms = project_row(w_mix_out, lax.all_gather(normed, "kv", axis=0, tiled=True))
    mixed = lax.psum(terms, "tp")
    after_mix = (rows_float + mixed).astype(jnp.bfloat16)
    layer_out = channel_mix(after_mix, model, ffn_gain, w_gate, w_up, w_down)
    return (layer_out, updated)


def pick_body(*args, n_kv, n_tp):
    residual, state = args[0], args[7]
    powers = n_kv & (n_kv - 1) == 0 and n_tp & (n_tp - 1) == 0 and n_tp > PAIR
    tiled = residual.shape[1] % LANES == 0 and state.shape[0] % 8 == 0
    body = fast_body if powers and tiled else plain_body
    return body(*args, n_kv=n_kv, n_tp=n_tp)


def solution(mesh):
    in_specs = (
        P(None, ("kv", "tp")),
        P("kv"),
        P("kv", "tp"),
        P("kv", "tp"),
        P("kv", "tp"),
        P("kv", "tp"),
        P("tp"),
        P("kv", "tp", None, None),
        P(),
        P("tp", "kv"),
        P("kv"),
        P("kv", "tp"),
        P("kv", "tp"),
        P("tp", "kv"),
    )
    out_specs = (P(None, ("kv", "tp")), P("kv", "tp", None, None))
    body = functools.partial(pick_body, n_kv=mesh.shape["kv"], n_tp=mesh.shape["tp"])
    return jax.shard_map(body, mesh=mesh, in_specs=in_specs, out_specs=out_specs, check_vma=False)
```

```python
import functools

import jax
import jax.numpy as jnp
from jax import lax
from jax.experimental import pallas as pl
from jax.experimental.pallas import tpu as pltpu
from jax.sharding import PartitionSpec as P

EPS = 1e-06
LANES = 128
PAIR = 2
BF16 = jnp.bfloat16
F32 = jnp.float32


def exchange(value, axis, size, mask):
    return lax.ppermute(value, axis, [(i, i ^ mask) for i in range(size)])


def call(kernel, outs, scratch=(), megabytes=8, space=pltpu.VMEM):
    inner = pl.pallas_call(
        kernel,
        out_shape=[space(shape, dtype) for shape, dtype in outs],
        scratch_shapes=list(scratch),
        compiler_params=pltpu.CompilerParams(vmem_limit_bytes=megabytes << 20),
    )
    return lambda *args: inner(
        *(pltpu.with_memory_space_constraint(arg, pltpu.VMEM) for arg in args)
    )


def tail_pieces(total, first_lane):
    lane = lax.broadcasted_iota(jnp.int32, (total.shape[0], LANES), 1) - first_lane
    high = total.astype(BF16).astype(F32)
    middle = (total - high).astype(BF16).astype(F32)
    low = total - high - middle
    zero = jnp.zeros((), F32)
    return jnp.where(
        lane == 0, high, jnp.where(lane == 1, middle, jnp.where(lane == 2, low, zero))
    )


def load_kernel(*refs):
    count = len(refs) // 2
    copies = [
        pltpu.make_async_copy(refs[i], refs[count + i], refs[-1].at[i]) for i in range(count)
    ]
    for copy in copies:
        copy.start()
    for copy in copies:
        copy.wait()


def load(*arrays):
    size = sum(a.size * a.dtype.itemsize for a in arrays)
    return pl.pallas_call(
        load_kernel,
        in_specs=[pl.BlockSpec(memory_space=pltpu.HBM)] * len(arrays),
        out_specs=[pl.BlockSpec(memory_space=pltpu.VMEM)] * len(arrays),
        out_shape=[pltpu.VMEM(a.shape, a.dtype) for a in arrays],
        scratch_shapes=[pltpu.SemaphoreType.DMA((len(arrays),))],
        cost_estimate=pl.CostEstimate(flops=16 * size, bytes_accessed=2 * size, transcendentals=0),
        compiler_params=pltpu.CompilerParams(vmem_limit_bytes=1 << 20),
    )(*(pltpu.with_memory_space_constraint(a, pltpu.HBM) for a in arrays))


def product(left, right, right_dim=0):
    dims = (((1,), (right_dim,)), ((), ()))
    return lax.dot_general(left, right, dims, preferred_element_type=F32)


def gather_scaled(near_ref, far_ref, gain_ref, blocks_ref, count):
    own = lax.axis_index("tp")
    squares = None
    for k in range(count):
        for ref, source in ((near_ref, own ^ (PAIR * k)), (far_ref, own ^ (PAIR * k + 1))):
            block = ref[k].astype(F32)
            squares = block * block if squares is None else squares + block * block
            blocks_ref[source] = (block * gain_ref[source]).astype(BF16)
    rows = jnp.concatenate([blocks_ref[j] for j in range(PAIR * count)], axis=1)
    return rows, jnp.sum(squares, axis=1, keepdims=True)


def spread(parts_ref, own_ref, send_refs):
    own = lax.axis_index("kv")
    own_ref[...] = parts_ref[own]
    for mask, ref in enumerate(send_refs, 1):
        ref[...] = parts_ref[own ^ mask].astype(BF16)


def project_kernel(near_ref, far_ref, gain_ref, *refs, count, n_weights, offsets, tail, local, dim):
    weights, outs = refs[:n_weights], refs[n_weights:-2]
    blocks_ref, parts_ref = refs[-2:]
    rows, squares = gather_scaled(near_ref, far_ref, gain_ref, blocks_ref, count)
    groups = parts_ref.shape[0]
    start = tail // LANES * LANES
    pieces = tail_pieces(squares, tail - start)

    def put(value, at):
        for d in range(groups):
            parts_ref[d, :, at : at + value.shape[1]] = value[d * local : (d + 1) * local]

    zero = jnp.zeros((rows.shape[0], LANES), F32)
    put(zero, parts_ref.shape[2] - LANES)
    put(pieces, start)
    for weight, at in zip(weights, offsets):
        put(product(rows, weight[...], dim), at)
    spread(parts_ref, outs[0], outs[1:])


def project(near, far, gains, weights, offsets, tail, width, n_kv, dim=0):
    count, seqs, block = near.shape
    local = seqs // n_kv
    kernel = functools.partial(
        project_kernel,
        count=count,
        n_weights=len(weights),
        offsets=offsets,
        tail=tail,
        local=local,
        dim=dim,
    )
    outs = [((local, width), F32)] + [((local, width), BF16)] * (n_kv - 1)
    scratch = [
        pltpu.VMEM((PAIR * count, seqs, block), BF16),
        pltpu.VMEM((n_kv, local, width), F32),
    ]
    return call(kernel, outs, scratch)(near, far, gains, *weights)


def halves(value):
    high = value.astype(BF16).astype(F32)
    return high, value - high


def diagonal(tile):
    row = lax.broadcasted_iota(jnp.int32, tile.shape, 0)
    return jnp.concatenate([jnp.where(row == s, tile, 0.0) for s in range(tile.shape[0])], axis=1)


def outer(left, right):
    left, right = jnp.concatenate(left, axis=0), jnp.concatenate(right, axis=0)
    dims = (((0,), (0,)), ((), ()))
    return lax.dot_general(left.astype(BF16), right.astype(BF16), dims, preferred_element_type=F32)


def gates(parts, bound_ref, model, hid, vid, span=slice(None)):
    raw = parts[0][span, :]
    for ref in parts[1:]:
        raw = raw + ref[span, :].astype(F32)
    total = jnp.sum(raw[:, -LANES:], axis=1, keepdims=True)
    raw = raw * lax.rsqrt(total / model + EPS)
    bound = bound_ref[...]
    forget_raw = raw[:, hid : 2 * hid]
    forget = bound + (1.0 - bound) * jax.nn.sigmoid(forget_raw)
    keyvec = (1.0 - bound) * jax.nn.sigmoid(-forget_raw)
    return raw, forget, keyvec, raw[:, 2 * hid : 2 * hid + vid]


def read_kernel(*refs, n_parts, model, step):
    parts = refs[:n_parts]
    bound_ref, gain_ref, state_ref, normed_ref = refs[n_parts:]
    local, heads, keys, values = state_ref.shape
    hid, vid = heads * keys, heads * values
    row = lax.broadcasted_iota(jnp.int32, (step, values), 0)
    raw, forget, keyvec, value = gates(parts, bound_ref, model, hid, vid)
    query = jax.nn.silu(raw[:, :hid])
    out_gate = jax.nn.silu(raw[:, 2 * hid + vid : 2 * (hid + vid)])
    for at in range(0, local, step):
        for h in range(heads):
            rows = slice(at, at + step)
            lanes = slice(h * keys, (h + 1) * keys)
            to = slice(h * values, (h + 1) * values)
            q, f, k = (v[rows, lanes] for v in (query, forget, keyvec))
            v = value[rows, to]
            old = jnp.concatenate([state_ref[s, h] for s in range(at, at + step)], axis=1)
            old = jnp.concatenate([piece.astype(BF16) for piece in halves(old)], axis=0)
            left = jnp.concatenate(halves(q * f), axis=0).astype(BF16)
            read = product(jnp.concatenate([left, left], axis=1), old)
            read = read[:step] + read[step:]
            head_out = jnp.sum(q * k, axis=1, keepdims=True) * v
            for s in range(step):
                head_out += jnp.where(row == s, read[:, s * values : (s + 1) * values], 0.0)
            scale = lax.rsqrt(jnp.mean(head_out * head_out, axis=1, keepdims=True) + EPS)
            normed = head_out * scale * gain_ref[...] * out_gate[rows, to]
            normed_ref[rows, to] = normed.astype(BF16)


def update_kernel(*refs, n_parts, model, step):
    parts = refs[:n_parts]
    bound_ref, state_ref, _, new_ref, token_ref = refs[n_parts:]
    token_ref[...] = jnp.zeros(token_ref.shape, F32)
    _, heads, keys, values = state_ref.shape
    hid, vid = heads * keys, heads * values
    start = pl.multiple_of(pl.program_id(0) * step, step)
    _, forget, keyvec, value = gates(parts, bound_ref, model, hid, vid, pl.ds(start, step))
    ones = diagonal(jnp.ones((step, values), F32))
    for h in range(heads):
        lanes = slice(h * keys, (h + 1) * keys)
        to = slice(h * values, (h + 1) * values)
        decay = outer(halves(forget[:, lanes]), (ones, ones))
        k_high, k_low = halves(keyvec[:, lanes])
        v_high, v_low = (diagonal(piece) for piece in halves(value[:, to]))
        added = outer((k_high, k_high, k_low, k_low), (v_high, v_low, v_high, v_low))
        for s in range(step):
            cols = slice(s * values, (s + 1) * values)
            new_ref[s, h] = decay[:, cols] * state_ref[start + s, h] + added[:, cols]


def read_state(parts, bound, head_gain, state, model):
    local, heads, _, values = state.shape
    kernel = functools.partial(read_kernel, n_parts=len(parts), model=model, step=8)
    outs = [((local, heads * values), BF16)]
    return call(kernel, outs, megabytes=12)(*parts, bound, head_gain.reshape(1, values), state)[0]


def update_state(parts, bound, state, model, after):
    local, heads, keys, values = state.shape
    step = 8
    kernel = functools.partial(update_kernel, n_parts=len(parts), model=model, step=step)
    whole = pl.BlockSpec(memory_space=pltpu.VMEM)
    args = *parts, bound, state, after
    return pl.pallas_call(
        kernel,
        grid=(local // step,),
        in_specs=[whole] * len(args),
        out_specs=[
            pl.BlockSpec((step, heads, keys, values), lambda i: (i, 0, 0, 0)),
            whole,
        ],
        out_shape=[jax.ShapeDtypeStruct(state.shape, F32), pltpu.VMEM((8, LANES), F32)],
        cost_estimate=pl.CostEstimate(
            flops=64 * state.size, bytes_accessed=8 * state.size, transcendentals=0
        ),
        compiler_params=pltpu.CompilerParams(vmem_limit_bytes=12 << 20),
    )(*(pltpu.with_memory_space_constraint(v, pltpu.VMEM) for v in args))


def mix_kernel(*refs, n_parts, local, count):
    parts = refs[:n_parts]
    weight_ref, keep_ref, send_ref, rows_ref, terms_ref = refs[n_parts:]
    own = lax.axis_index("kv")
    core = lax.axis_index("tp") % PAIR
    depth = weight_ref.shape[0]
    for mask, ref in enumerate(parts):
        rows_ref[own ^ mask] = ref[...]
    rows = jnp.concatenate([rows_ref[d] for d in range(n_parts)], axis=0)
    terms = product(rows[:, :depth], weight_ref[...])
    block = terms.shape[1] // (PAIR * count)
    for j in range(PAIR * count):
        terms_ref[j] = terms[:, j * block : (j + 1) * block]
    for z in range(count):
        keep_ref[z] = terms_ref[PAIR * z + core]
        send_ref[z] = terms_ref[PAIR * z + 1 - core].astype(BF16)


def mix(parts, weight, count):
    local, width = parts[0].shape
    n_kv = len(parts)
    seqs = local * n_kv
    block = weight.shape[1] // (PAIR * count)
    kernel = functools.partial(mix_kernel, n_parts=n_kv, local=local, count=count)
    outs = [((count, seqs, block), F32), ((count, seqs, block), BF16)]
    scratch = [
        pltpu.VMEM((n_kv, local, width), BF16),
        pltpu.VMEM((PAIR * count, seqs, block), F32),
    ]
    return call(kernel, outs, scratch)(*parts, weight)


def fold_kernel(keep_ref, far_ref, own_ref, *send_refs):
    z = lax.axis_index("tp") // PAIR
    own_ref[...] = keep_ref[z] + far_ref[z].astype(F32)
    for mask, ref in enumerate(send_refs, 1):
        ref[...] = (keep_ref[z ^ mask] + far_ref[z ^ mask].astype(F32)).astype(BF16)


def finish_kernel(base_ref, *refs):
    total = base_ref[...].astype(F32)
    for ref in refs[:-1]:
        total = total + ref[...].astype(F32)
    refs[-1][...] = total.astype(BF16)


def reduce_tp(keep, send, base, n_tp):
    count, seqs, block = keep.shape
    far = exchange(send, "tp", n_tp, 1)
    outs = [((seqs, block), F32)] + [((seqs, block), BF16)] * (count - 1)
    own, *sends = call(fold_kernel, outs)(keep, far)
    got = [exchange(v, "tp", n_tp, PAIR * k) for k, v in enumerate(sends, 1)]
    finish = call(finish_kernel, [((seqs, block), BF16)], space=jax.ShapeDtypeStruct)
    return finish(base, own, *got)[0]


def narrow_kernel(keep_ref, far_ref, own_ref, send_ref):
    for z in range(keep_ref.shape[0]):
        total = keep_ref[z] + far_ref[z].astype(F32)
        own_ref[z] = total
        send_ref[z] = total.astype(BF16)


def settle_kernel(near_ref, own_ref, *refs):
    count = own_ref.shape[0]
    z = lax.axis_index("tp") // PAIR
    for k in range(count):
        total = near_ref[k].astype(F32) + own_ref[z ^ k]
        for ref in refs[:-2]:
            total = total + ref[z ^ k].astype(F32)
        refs[-1][k] = total.astype(BF16)


def sum_tp(keep, send, near, update, n_tp):
    count, seqs, block = keep.shape
    far = exchange(send, "tp", n_tp, 1)
    shape = (count, seqs, block)
    own, narrow = call(narrow_kernel, [(shape, F32), (shape, BF16)])(keep, far)
    got = [exchange(narrow, "tp", n_tp, PAIR * k) for k in range(1, count)]
    updated, token = update(own)
    mine = call(settle_kernel, [(shape, BF16)])(near, own, *got, token)[0]
    return mine, exchange(mine, "tp", n_tp, 1), updated


def stack_kernel(*refs, count):
    for k in range(count):
        refs[-1][k] = refs[k][...]


def gather_tp(block, held, n_tp):
    count = n_tp // PAIR
    blocks = [held] + [exchange(block, "tp", n_tp, PAIR * k) for k in range(1, count)]
    kernel = functools.partial(stack_kernel, count=count)
    near = call(kernel, [((count, *block.shape), BF16)])(*blocks)[0]
    return near, exchange(near, "tp", n_tp, 1)


def hidden_kernel(*refs, model, tail):
    raw = refs[0][...]
    for ref in refs[1:-1]:
        raw = raw + ref[...].astype(F32)
    half = raw.shape[1] // 2
    start = tail // LANES * LANES
    lane = lax.broadcasted_iota(jnp.int32, (raw.shape[0], LANES), 1)
    pieces = jnp.where(lane >= tail - start, raw[:, start : start + LANES], 0.0)
    inverse = lax.rsqrt(jnp.sum(pieces, axis=1, keepdims=True) / model + EPS)
    gate = raw[:, :half] * inverse
    refs[-1][...] = (jax.nn.silu(gate) * (raw[:, half:] * inverse)).astype(BF16)


def fast_body(
    residual,
    mixer_gain,
    w_query,
    w_forget,
    w_input,
    w_outgate,
    lower_bound,
    state,
    head_gain,
    w_mix_out,
    ffn_gain,
    w_gate,
    w_up,
    w_down,
    *,
    n_kv,
    n_tp,
):
    count = n_tp // PAIR
    model = residual.shape[1] * n_kv * n_tp
    local = state.shape[0]
    kv_masks = range(1, n_kv)

    gains = mixer_gain.reshape(n_tp, 1, -1)
    gains, held, *weights = load(gains, residual, w_query, w_forget, w_input, w_outgate)
    near, far = gather_tp(residual, held, n_tp)
    offsets, at = [], 0
    for weight in weights:
        offsets.append(at)
        at += weight.shape[1]
    own, *sends = project(near, far, gains, weights, offsets, at, at + LANES, n_kv)
    (held,) = load(state)
    parts = [own] + [exchange(v, "kv", n_kv, m) for m, v in zip(kv_masks, sends)]
    bound = lower_bound.reshape(1, -1)
    normed = read_state(parts, bound, head_gain, held, model)

    rows = [normed] + [exchange(normed, "kv", n_kv, m) for m in kv_masks]
    keep, send = mix(rows, w_mix_out, count)
    update = functools.partial(update_state, parts, bound, held, model)
    near, far, new_state = sum_tp(keep, send, near, update, n_tp)
    after_mix = near[0]

    units = w_gate.shape[1]
    padded = (units + 3 + LANES - 1) // LANES * LANES
    own, *sends = project(
        near, far, ffn_gain.reshape(n_tp, 1, -1), (w_gate.T, w_up.T), (0, padded), units, 2 * padded, n_kv, 1
    )
    parts = [own] + [exchange(v, "kv", n_kv, m) for m, v in zip(kv_masks, sends)]
    kernel = functools.partial(hidden_kernel, model=model, tail=units)
    hidden = call(kernel, [((local, padded), BF16)])(*parts)[0]
    parts = [hidden] + [exchange(hidden, "kv", n_kv, m) for m in kv_masks]
    keep, send = mix(parts, w_down, count)
    return reduce_tp(keep, send, after_mix, n_tp), new_state


def project_row(weight, piece):
    return jnp.dot(piece, weight, preferred_element_type=jnp.float32)


def channel_mix(rows_in, model, ffn_gain, w_gate, w_up, w_down):
    rows_float = rows_in.astype(jnp.float32)
    squares = jnp.sum(rows_float * rows_float, axis=1)
    scaled = (rows_float * ffn_gain).astype(jnp.bfloat16)
    gate = jnp.dot(scaled, w_gate, preferred_element_type=jnp.float32)
    upper = jnp.dot(scaled, w_up, preferred_element_type=jnp.float32)
    whole_total = lax.psum(squares, "kv")
    gate, upper = (
        lax.psum(gate.astype(jnp.bfloat16), "kv").astype(jnp.float32),
        lax.psum(upper.astype(jnp.bfloat16), "kv").astype(jnp.float32),
    )
    inverse = lax.rsqrt(whole_total / model + EPS)[:, None]
    hidden = (jax.nn.silu(gate * inverse) * (upper * inverse)).astype(jnp.bfloat16)
    terms = jnp.dot(hidden, w_down, preferred_element_type=jnp.float32)
    summed = lax.psum_scatter(
        terms.astype(jnp.bfloat16), "tp", scatter_dimension=1, tiled=True
    ).astype(jnp.float32)
    width = summed.shape[1]
    own = lax.dynamic_slice_in_dim(rows_float, lax.axis_index("tp") * width, width, 1)
    return (own + summed).astype(jnp.bfloat16)


def plain_body(
    residual,
    mixer_gain,
    w_query,
    w_forget,
    w_input,
    w_outgate,
    lower_bound,
    state,
    head_gain,
    w_mix_out,
    ffn_gain,
    w_gate,
    w_up,
    w_down,
    *,
    n_kv,
    n_tp,
):
    local_seqs, local_heads, DK, DV = state.shape
    model = residual.shape[1] * n_kv * n_tp
    rows = lax.all_gather(residual, "tp", axis=1, tiled=True)
    rows_float = rows.astype(jnp.float32)
    squares = jnp.sum(rows_float * rows_float, axis=1)
    scaled = (rows_float * mixer_gain).astype(jnp.bfloat16)
    part_query = jnp.dot(scaled, w_query, preferred_element_type=jnp.float32)
    part_forget = jnp.dot(scaled, w_forget, preferred_element_type=jnp.float32)
    part_value = jnp.dot(scaled, w_input, preferred_element_type=jnp.float32)
    part_gate = jnp.dot(scaled, w_outgate, preferred_element_type=jnp.float32)
    whole_total = lax.psum(squares, "kv")
    total = lax.dynamic_slice_in_dim(whole_total, lax.axis_index("kv") * local_seqs, local_seqs)
    part_query, part_forget, part_value, part_gate = (
        lax.psum_scatter(part_query, "kv", scatter_dimension=0, tiled=True),
        lax.psum_scatter(part_forget, "kv", scatter_dimension=0, tiled=True),
        lax.psum_scatter(part_value, "kv", scatter_dimension=0, tiled=True),
        lax.psum_scatter(part_gate, "kv", scatter_dimension=0, tiled=True),
    )
    inverse = lax.rsqrt(total / model + EPS)[:, None]
    bound = lower_bound.reshape(local_heads, DK)
    forget_raw = (part_forget * inverse).reshape(local_seqs, local_heads, DK)
    forget = bound + (1.0 - bound) * jax.nn.sigmoid(forget_raw)
    keyvec = (1.0 - bound) * jax.nn.sigmoid(-forget_raw)
    query = jax.nn.silu((part_query * inverse).reshape(local_seqs, local_heads, DK))
    values = (part_value * inverse).reshape(local_seqs, local_heads, DV)
    updated = forget[..., None] * state + keyvec[..., None] * values[:, :, None, :]
    head_out = jnp.einsum("shc,shce->she", query, updated, precision=lax.Precision.HIGHEST)
    inv_head = lax.rsqrt(jnp.mean(head_out * head_out, axis=2, keepdims=True) + EPS)
    out_gate = jax.nn.silu((part_gate * inverse).reshape(local_seqs, local_heads, DV))
    normed = (
        (head_out * inv_head * head_gain * out_gate)
        .reshape(local_seqs, local_heads * DV)
        .astype(jnp.bfloat16)
    )
    terms = project_row(w_mix_out, lax.all_gather(normed, "kv", axis=0, tiled=True))
    mixed = lax.psum(terms, "tp")
    after_mix = (rows_float + mixed).astype(jnp.bfloat16)
    layer_out = channel_mix(after_mix, model, ffn_gain, w_gate, w_up, w_down)
    return (layer_out, updated)


def pick_body(*args, n_kv, n_tp):
    residual, state = args[0], args[7]
    powers = n_kv & (n_kv - 1) == 0 and n_tp & (n_tp - 1) == 0 and n_tp > PAIR
    tiled = residual.shape[1] % LANES == 0 and state.shape[0] % 8 == 0
    body = fast_body if powers and tiled else plain_body
    return body(*args, n_kv=n_kv, n_tp=n_tp)


def solution(mesh):
    in_specs = (
        P(None, ("kv", "tp")),
        P("kv"),
        P("kv", "tp"),
        P("kv", "tp"),
        P("kv", "tp"),
        P("kv", "tp"),
        P("tp"),
        P("kv", "tp", None, None),
        P(),
        P("tp", "kv"),
        P("kv"),
        P("kv", "tp"),
        P("kv", "tp"),
        P("tp", "kv"),
    )
    out_specs = (P(None, ("kv", "tp")), P("kv", "tp", None, None))
    body = functools.partial(pick_body, n_kv=mesh.shape["kv"], n_tp=mesh.shape["tp"])
    return jax.shard_map(body, mesh=mesh, in_specs=in_specs, out_specs=out_specs, check_vma=False)
```

```python
import functools

import jax
import jax.numpy as jnp
from jax import lax
from jax.experimental import pallas as pl
from jax.experimental.pallas import tpu as pltpu
from jax.sharding import PartitionSpec as P


EPS = 1e-06
LANES = 128
PAIR = 2
HALVES = 2
BF16 = jnp.bfloat16
F32 = jnp.float32


def exchange(value, axis, size, mask):
    return lax.ppermute(value, axis, [(i, i ^ mask) for i in range(size)])


def call(kernel, outs, scratch=(), megabytes=8, space=pltpu.VMEM):
    inner = pl.pallas_call(
        kernel,
        out_shape=[space(shape, dtype) for shape, dtype in outs],
        scratch_shapes=list(scratch),
        compiler_params=pltpu.CompilerParams(vmem_limit_bytes=megabytes << 20),
    )
    return lambda *args: inner(
        *(pltpu.with_memory_space_constraint(arg, pltpu.VMEM) for arg in args)
    )


def tail_pieces(total, first_lane):
    lane = lax.broadcasted_iota(jnp.int32, (total.shape[0], LANES), 1) - first_lane
    high = total.astype(BF16).astype(F32)
    middle = (total - high).astype(BF16).astype(F32)
    low = total - high - middle
    zero = jnp.zeros((), F32)
    return jnp.where(
        lane == 0, high, jnp.where(lane == 1, middle, jnp.where(lane == 2, low, zero))
    )


def load_kernel(*refs):
    count = len(refs) // 2
    copies = [
        pltpu.make_async_copy(refs[i], refs[count + i], refs[-1].at[i]) for i in range(count)
    ]
    for copy in copies:
        copy.start()
    for copy in copies:
        copy.wait()


def load(*arrays):
    size = sum(a.size * a.dtype.itemsize for a in arrays)
    return pl.pallas_call(
        load_kernel,
        in_specs=[pl.BlockSpec(memory_space=pltpu.HBM)] * len(arrays),
        out_specs=[pl.BlockSpec(memory_space=pltpu.VMEM)] * len(arrays),
        out_shape=[pltpu.VMEM(a.shape, a.dtype) for a in arrays],
        scratch_shapes=[pltpu.SemaphoreType.DMA((len(arrays),))],
        cost_estimate=pl.CostEstimate(flops=16 * size, bytes_accessed=2 * size, transcendentals=0),
        compiler_params=pltpu.CompilerParams(vmem_limit_bytes=1 << 20),
    )(*(pltpu.with_memory_space_constraint(a, pltpu.HBM) for a in arrays))


def product(left, right, right_dim=0):
    dims = (((1,), (right_dim,)), ((), ()))
    return lax.dot_general(left, right, dims, preferred_element_type=F32)


def scaled_rows(blocks_ref, gains_ref, shift, local):
    own, here = lax.axis_index("tp"), lax.axis_index("kv")
    spans = [
        pl.ds(pl.multiple_of((here ^ mask) * local, local), local)
        for mask in range(blocks_ref.shape[1] // local)
    ]
    sources = [own ^ (PAIR * k + shift) for k in range(blocks_ref.shape[0])]
    squares, rows = None, []
    for k, source in enumerate(sources):
        block = jnp.concatenate([blocks_ref[k, span, :] for span in spans], axis=0).astype(F32)
        squares = block * block if squares is None else squares + block * block
        rows.append((block * gains_ref[source]).astype(BF16))
    return jnp.concatenate(rows, axis=1), sources, squares


def feature_slices(weight_ref, sources, block, dim):
    spans = [pl.ds(pl.multiple_of(source * block, block), block) for source in sources]
    return jnp.concatenate([weight_ref[(slice(None),) * dim + (at,)] for at in spans], axis=dim)


def near_kernel(near_ref, gains_ref, *refs, n_weights, local, dim):
    weights, outs, squares_ref = refs[:n_weights], refs[n_weights:-1], refs[-1]
    rows, sources, squares = scaled_rows(near_ref, gains_ref, 0, local)
    squares_ref[...] = squares
    for weight, out in zip(weights, outs):
        out[...] = product(rows, feature_slices(weight, sources, near_ref.shape[2], dim), dim)


def far_kernel(far_ref, gains_ref, near_squares_ref, *refs, offsets, tail, local, dim):
    n_weights = len(offsets)
    weights, nears = refs[:n_weights], refs[n_weights : 2 * n_weights]
    outs = refs[2 * n_weights :]
    rows, sources, squares = scaled_rows(far_ref, gains_ref, 1, local)
    width = outs[0].shape[1]

    def put(value, at):
        for mask, out in enumerate(outs):
            part = value[mask * local : (mask + 1) * local]
            out[:, at : at + value.shape[1]] = part.astype(out.dtype)

    put(jnp.zeros((rows.shape[0], LANES), F32), width - LANES)
    squares = jnp.sum(squares + near_squares_ref[...], axis=1, keepdims=True)
    start = tail // LANES * LANES
    put(tail_pieces(squares, tail - start), start)
    for weight, near, at in zip(weights, nears, offsets):
        slices = feature_slices(weight, sources, far_ref.shape[2], dim)
        put(near[...] + product(rows, slices, dim), at)


def project(near, far, gains, weights, offsets, tail, width, n_kv, dim=0):
    _, seqs, block = near.shape
    local = seqs // n_kv
    kernel = functools.partial(near_kernel, n_weights=len(weights), local=local, dim=dim)
    outs = [((seqs, weight.shape[1 - dim]), F32) for weight in weights] + [((seqs, block), F32)]
    *halfway, squares = call(kernel, outs)(near, gains, *weights)
    kernel = functools.partial(far_kernel, offsets=offsets, tail=tail, local=local, dim=dim)
    outs = [((local, width), F32)] + [((local, width), BF16)] * (n_kv - 1)
    own, *sends = call(kernel, outs)(far, gains, squares, *weights, *halfway)
    return [own] + [exchange(v, "kv", n_kv, m) for m, v in enumerate(sends, 1)]


def halves(value):
    high = value.astype(BF16).astype(F32)
    return high, value - high


def diagonal(tile):
    row = lax.broadcasted_iota(jnp.int32, tile.shape, 0)
    return jnp.concatenate([jnp.where(row == s, tile, 0.0) for s in range(tile.shape[0])], axis=1)


def outer(left, right):
    left, right = jnp.concatenate(left, axis=0), jnp.concatenate(right, axis=0)
    dims = (((0,), (0,)), ((), ()))
    return lax.dot_general(left.astype(BF16), right.astype(BF16), dims, preferred_element_type=F32)


def gates(parts, bound_ref, model, hid, vid, span=slice(None)):
    raw = parts[0][span, :]
    for ref in parts[1:]:
        raw = raw + ref[span, :].astype(F32)
    total = jnp.sum(raw[:, -LANES:], axis=1, keepdims=True)
    raw = raw * lax.rsqrt(total / model + EPS)
    bound = bound_ref[...]
    forget_raw = raw[:, hid : 2 * hid]
    forget = bound + (1.0 - bound) * jax.nn.sigmoid(forget_raw)
    keyvec = (1.0 - bound) * jax.nn.sigmoid(-forget_raw)
    return raw, forget, keyvec, raw[:, 2 * hid : 2 * hid + vid]


def read_kernel(*refs, n_parts, model, step):
    parts = refs[:n_parts]
    bound_ref, gain_ref, state_ref, normed_ref = refs[n_parts:]
    local, heads, keys, values = state_ref.shape
    hid, vid = heads * keys, heads * values
    row = lax.broadcasted_iota(jnp.int32, (step, values), 0)
    raw, forget, keyvec, value = gates(parts, bound_ref, model, hid, vid)
    query = jax.nn.silu(raw[:, :hid])
    out_gate = jax.nn.silu(raw[:, 2 * hid + vid : 2 * (hid + vid)])
    for at in range(0, local, step):
        for h in range(heads):
            rows = slice(at, at + step)
            lanes = slice(h * keys, (h + 1) * keys)
            to = slice(h * values, (h + 1) * values)
            q, f, k = (v[rows, lanes] for v in (query, forget, keyvec))
            v = value[rows, to]
            old = jnp.concatenate([state_ref[s, h] for s in range(at, at + step)], axis=1)
            left = jnp.concatenate(halves(q * f), axis=0).astype(BF16)
            read = product(left, old.astype(BF16))
            read = read[:step] + read[step:]
            head_out = jnp.sum(q * k, axis=1, keepdims=True) * v
            for s in range(step):
                head_out += jnp.where(row == s, read[:, s * values : (s + 1) * values], 0.0)
            scale = lax.rsqrt(jnp.mean(head_out * head_out, axis=1, keepdims=True) + EPS)
            normed = head_out * scale * gain_ref[...] * out_gate[rows, to]
            normed_ref[rows, to] = normed.astype(BF16)


def update_kernel(*refs, n_parts, model, step, first):
    parts = refs[:n_parts]
    bound_ref, state_ref, *_, new_ref, token_ref = refs[n_parts:]
    token_ref[...] = jnp.zeros(token_ref.shape, F32)
    _, heads, keys, values = state_ref.shape
    hid, vid = heads * keys, heads * values
    start = pl.multiple_of((first + pl.program_id(0)) * step, step)
    _, forget, keyvec, value = gates(parts, bound_ref, model, hid, vid, pl.ds(start, step))
    ones = diagonal(jnp.ones((step, values), F32))
    for h in range(heads):
        lanes = slice(h * keys, (h + 1) * keys)
        to = slice(h * values, (h + 1) * values)
        decay = outer(halves(forget[:, lanes]), (ones, ones))
        k_high, k_low = halves(keyvec[:, lanes])
        v_high, v_low = (diagonal(piece) for piece in halves(value[:, to]))
        added = outer((k_high, k_high, k_low, k_low), (v_high, v_low, v_high, v_low))
        for s in range(step):
            cols = slice(s * values, (s + 1) * values)
            new_ref[s, h] = decay[:, cols] * state_ref[start + s, h] + added[:, cols]


def read_state(parts, bound, head_gain, state, model):
    local, heads, _, values = state.shape
    kernel = functools.partial(read_kernel, n_parts=len(parts), model=model, step=8)
    outs = [((local, heads * values), BF16)]
    return call(kernel, outs, megabytes=12)(*parts, bound, head_gain.reshape(1, values), state)[0]


def update_state(parts, bound, state, model, part, after, partial=None):
    local, heads, keys, values = state.shape
    step = 8
    steps = local // step // HALVES
    kernel = functools.partial(
        update_kernel, n_parts=len(parts), model=model, step=step, first=part * steps
    )
    whole = pl.BlockSpec(memory_space=pltpu.VMEM)
    args = [pltpu.with_memory_space_constraint(v, pltpu.VMEM) for v in (*parts, bound, state, after)]
    specs, aliases = [whole] * len(args), {}
    if partial is not None:
        aliases[len(args)] = 0
        args.append(partial)
        specs.append(pl.BlockSpec(memory_space=pl.ANY))
    return pl.pallas_call(
        kernel,
        grid=(steps,),
        in_specs=specs,
        out_specs=[
            pl.BlockSpec((step, heads, keys, values), lambda i: (part * steps + i, 0, 0, 0)),
            whole,
        ],
        out_shape=[jax.ShapeDtypeStruct(state.shape, F32), pltpu.VMEM((8, LANES), F32)],
        input_output_aliases=aliases,
        cost_estimate=pl.CostEstimate(
            flops=32 * state.size, bytes_accessed=4 * state.size, transcendentals=0
        ),
        compiler_params=pltpu.CompilerParams(vmem_limit_bytes=12 << 20),
    )(*args)


def mix_kernel(*refs, n_parts, flip):
    parts = refs[:n_parts]
    weight_ref, *_, out_ref, rows_ref = refs[n_parts:]
    own = lax.axis_index("kv")
    core = lax.axis_index("tp") % PAIR ^ flip
    count, _, block = out_ref.shape
    for mask, ref in enumerate(parts):
        rows_ref[own ^ mask] = ref[...]
    rows = jnp.concatenate([rows_ref[d] for d in range(n_parts)], axis=0)
    columns = feature_slices(weight_ref, [PAIR * z + core for z in range(count)], block, 1)
    terms = product(rows[:, : weight_ref.shape[0]], columns)
    for z in range(count):
        out_ref[z] = terms[:, z * block : (z + 1) * block].astype(out_ref.dtype)


def mix(parts, weight, count, *before):
    local, width = parts[0].shape
    n_kv = len(parts)
    shape = (count, local * n_kv, weight.shape[1] // (PAIR * count))
    scratch = [pltpu.VMEM((n_kv, local, width), BF16)]

    def half(flip, dtype):
        kernel = functools.partial(mix_kernel, n_parts=n_kv, flip=flip)
        return call(kernel, [(shape, dtype)], scratch)(*parts, weight, *before)[0]

    return half(0, F32), half(1, BF16)


def fold_kernel(keep_ref, far_ref, own_ref, *send_refs):
    z = lax.axis_index("tp") // PAIR
    own_ref[...] = keep_ref[z] + far_ref[z].astype(F32)
    for mask, ref in enumerate(send_refs, 1):
        ref[...] = (keep_ref[z ^ mask] + far_ref[z ^ mask].astype(F32)).astype(BF16)


def finish_kernel(*refs, local):
    bases, refs = refs[:HALVES], refs[HALVES:]
    step = local // HALVES
    rows = refs[0].shape[0] // HALVES
    spans = [(h, at) for at in range(0, rows, step) for h in range(HALVES)]
    base = jnp.concatenate([bases[h][0, at : at + step, :] for h, at in spans], axis=0)
    total = base.astype(F32)
    for ref in refs[:-1]:
        total = total + ref[...].astype(F32)
    refs[-1][...] = total.astype(BF16)


def reduce_tp(keep, send, bases, local, n_tp):
    count, seqs, block = keep.shape
    far = exchange(send, "tp", n_tp, 1)
    outs = [((seqs, block), F32)] + [((seqs, block), BF16)] * (count - 1)
    own, *sends = call(fold_kernel, outs)(keep, far)
    got = [exchange(v, "tp", n_tp, PAIR * k) for k, v in enumerate(sends, 1)]
    kernel = functools.partial(finish_kernel, local=local)
    finish = call(kernel, [((seqs, block), BF16)], space=jax.ShapeDtypeStruct)
    return finish(*bases, own, *got)[0]


def half_rows(value, half, local):
    step = local // HALVES
    starts = range(half * step, value.shape[0], local)
    return jnp.concatenate([value[at : at + step] for at in starts], axis=0)


def narrow_kernel(keep_ref, far_ref, *refs, local):
    for z in range(keep_ref.shape[0]):
        total = keep_ref[z] + far_ref[z].astype(F32)
        for h in range(HALVES):
            rows = half_rows(total, h, local)
            refs[h][z] = rows
            refs[HALVES + h][z] = rows.astype(BF16)


def settle_kernel(near_ref, own_ref, *refs, half, local):
    count = own_ref.shape[0]
    z = lax.axis_index("tp") // PAIR
    for k in range(count):
        total = half_rows(near_ref[k], half, local).astype(F32) + own_ref[z ^ k]
        for ref in refs[:-1]:
            total = total + ref[z ^ k].astype(F32)
        refs[-1][k] = total.astype(BF16)


def stack_kernel(*refs, count):
    for k in range(count):
        refs[-1][k] = refs[k][...]


def gather_tp(block, held, n_tp):
    count = n_tp // PAIR
    blocks = [held] + [exchange(block, "tp", n_tp, PAIR * k) for k in range(1, count)]
    kernel = functools.partial(stack_kernel, count=count)
    near = call(kernel, [((count, *block.shape), BF16)])(*blocks)[0]
    return near, exchange(near, "tp", n_tp, 1)


def hidden_kernel(*refs, model, tail, n_parts):
    start = tail // LANES * LANES
    step = refs[0].shape[0]
    for h in range(HALVES):
        parts = refs[h * n_parts : (h + 1) * n_parts]
        raw = parts[0][...]
        for ref in parts[1:]:
            raw = raw + ref[...].astype(F32)
        half = raw.shape[1] // 2
        lane = lax.broadcasted_iota(jnp.int32, (step, LANES), 1)
        pieces = jnp.where(lane >= tail - start, raw[:, start : start + LANES], 0.0)
        inverse = lax.rsqrt(jnp.sum(pieces, axis=1, keepdims=True) / model + EPS)
        gate = raw[:, :half] * inverse
        value = jax.nn.silu(gate) * (raw[:, half:] * inverse)
        refs[-1][h * step : (h + 1) * step, :] = value.astype(BF16)


def fast_body(
    residual,
    mixer_gain,
    w_query,
    w_forget,
    w_input,
    w_outgate,
    lower_bound,
    state,
    head_gain,
    w_mix_out,
    ffn_gain,
    w_gate,
    w_up,
    w_down,
    *,
    n_kv,
    n_tp,
):
    count = n_tp // PAIR
    model = residual.shape[1] * n_kv * n_tp
    local = state.shape[0]
    kv_masks = range(1, n_kv)

    gains = mixer_gain.reshape(n_tp, 1, -1)
    gains, held, *weights = load(gains, residual, w_query, w_forget, w_input, w_outgate)
    near, far = gather_tp(residual, held, n_tp)
    offsets, width = [], 0
    for weight in weights:
        offsets.append(width)
        width += weight.shape[1]
    parts = project(near, far, gains, weights, offsets, width, width + LANES, n_kv)
    (held,) = load(state)
    bound = lower_bound.reshape(1, -1)
    normed = read_state(parts, bound, head_gain, held, model)

    rows = [normed] + [exchange(normed, "kv", n_kv, m) for m in kv_masks]
    keep, send = mix(rows, w_mix_out, count)
    far = exchange(send, "tp", n_tp, 1)
    shape = (count, keep.shape[1] // HALVES, keep.shape[2])
    kernel = functools.partial(narrow_kernel, local=local)
    outs = [(shape, F32)] * HALVES + [(shape, BF16)] * HALVES
    narrow = call(kernel, outs)(keep, far)
    sums = [
        [exchange(narrow[HALVES + h], "tp", n_tp, PAIR * k) for k in range(1, count)]
        for h in range(HALVES)
    ]

    units = w_gate.shape[1]
    padded = (units + 3 + LANES - 1) // LANES * LANES
    gains = ffn_gain.reshape(n_tp, 1, -1)
    weights = w_gate.T, w_up.T
    mines, received = [], []
    for h in range(HALVES):
        kernel = functools.partial(settle_kernel, half=h, local=local)
        mine = call(kernel, [(shape, BF16)])(near, narrow[h], *sums[h])[0]
        mines.append(mine)
        far = exchange(mine, "tp", n_tp, 1)
        offsets, wide = (0, padded), 2 * padded
        received += project(mine, far, gains, weights, offsets, units, wide, n_kv, 1)
    update = functools.partial(update_state, parts, bound, held, model)
    new_state, token = update(0, received[n_kv])
    kernel = functools.partial(hidden_kernel, model=model, tail=units, n_parts=n_kv)
    hidden = call(kernel, [((local, padded), BF16)])(*received, token)[0]
    rows = [hidden] + [exchange(hidden, "kv", n_kv, m) for m in kv_masks]
    new_state, token = update(1, hidden, new_state)
    keep, send = mix(rows, w_down, count, token)
    return reduce_tp(keep, send, mines, local, n_tp), new_state


def project_row(weight, piece):
    return jnp.dot(piece, weight, preferred_element_type=jnp.float32)


def channel_mix(rows_in, model, ffn_gain, w_gate, w_up, w_down):
    rows_float = rows_in.astype(jnp.float32)
    squares = jnp.sum(rows_float * rows_float, axis=1)
    scaled = (rows_float * ffn_gain).astype(jnp.bfloat16)
    gate = jnp.dot(scaled, w_gate, preferred_element_type=jnp.float32)
    upper = jnp.dot(scaled, w_up, preferred_element_type=jnp.float32)
    whole_total = lax.psum(squares, "kv")
    gate, upper = (
        lax.psum(gate.astype(jnp.bfloat16), "kv").astype(jnp.float32),
        lax.psum(upper.astype(jnp.bfloat16), "kv").astype(jnp.float32),
    )
    inverse = lax.rsqrt(whole_total / model + EPS)[:, None]
    hidden = (jax.nn.silu(gate * inverse) * (upper * inverse)).astype(jnp.bfloat16)
    terms = jnp.dot(hidden, w_down, preferred_element_type=jnp.float32)
    summed = lax.psum_scatter(
        terms.astype(jnp.bfloat16), "tp", scatter_dimension=1, tiled=True
    ).astype(jnp.float32)
    width = summed.shape[1]
    own = lax.dynamic_slice_in_dim(rows_float, lax.axis_index("tp") * width, width, 1)
    return (own + summed).astype(jnp.bfloat16)


def plain_body(
    residual,
    mixer_gain,
    w_query,
    w_forget,
    w_input,
    w_outgate,
    lower_bound,
    state,
    head_gain,
    w_mix_out,
    ffn_gain,
    w_gate,
    w_up,
    w_down,
    *,
    n_kv,
    n_tp,
):
    local_seqs, local_heads, DK, DV = state.shape
    model = residual.shape[1] * n_kv * n_tp
    rows = lax.all_gather(residual, "tp", axis=1, tiled=True)
    rows_float = rows.astype(jnp.float32)
    squares = jnp.sum(rows_float * rows_float, axis=1)
    scaled = (rows_float * mixer_gain).astype(jnp.bfloat16)
    part_query = jnp.dot(scaled, w_query, preferred_element_type=jnp.float32)
    part_forget = jnp.dot(scaled, w_forget, preferred_element_type=jnp.float32)
    part_value = jnp.dot(scaled, w_input, preferred_element_type=jnp.float32)
    part_gate = jnp.dot(scaled, w_outgate, preferred_element_type=jnp.float32)
    whole_total = lax.psum(squares, "kv")
    total = lax.dynamic_slice_in_dim(whole_total, lax.axis_index("kv") * local_seqs, local_seqs)
    part_query, part_forget, part_value, part_gate = (
        lax.psum_scatter(part_query, "kv", scatter_dimension=0, tiled=True),
        lax.psum_scatter(part_forget, "kv", scatter_dimension=0, tiled=True),
        lax.psum_scatter(part_value, "kv", scatter_dimension=0, tiled=True),
        lax.psum_scatter(part_gate, "kv", scatter_dimension=0, tiled=True),
    )
    inverse = lax.rsqrt(total / model + EPS)[:, None]
    bound = lower_bound.reshape(local_heads, DK)
    forget_raw = (part_forget * inverse).reshape(local_seqs, local_heads, DK)
    forget = bound + (1.0 - bound) * jax.nn.sigmoid(forget_raw)
    keyvec = (1.0 - bound) * jax.nn.sigmoid(-forget_raw)
    query = jax.nn.silu((part_query * inverse).reshape(local_seqs, local_heads, DK))
    values = (part_value * inverse).reshape(local_seqs, local_heads, DV)
    updated = forget[..., None] * state + keyvec[..., None] * values[:, :, None, :]
    head_out = jnp.einsum("shc,shce->she", query, updated, precision=lax.Precision.HIGHEST)
    inv_head = lax.rsqrt(jnp.mean(head_out * head_out, axis=2, keepdims=True) + EPS)
    out_gate = jax.nn.silu((part_gate * inverse).reshape(local_seqs, local_heads, DV))
    normed = (
        (head_out * inv_head * head_gain * out_gate)
        .reshape(local_seqs, local_heads * DV)
        .astype(jnp.bfloat16)
    )
    terms = project_row(w_mix_out, lax.all_gather(normed, "kv", axis=0, tiled=True))
    mixed = lax.psum(terms, "tp")
    after_mix = (rows_float + mixed).astype(jnp.bfloat16)
    layer_out = channel_mix(after_mix, model, ffn_gain, w_gate, w_up, w_down)
    return (layer_out, updated)


def pick_body(*args, n_kv, n_tp):
    residual, state = args[0], args[7]
    powers = n_kv & (n_kv - 1) == 0 and n_tp & (n_tp - 1) == 0 and n_tp > PAIR
    tiled = residual.shape[1] % LANES == 0 and state.shape[0] % 8 == 0
    body = fast_body if powers and tiled else plain_body
    return body(*args, n_kv=n_kv, n_tp=n_tp)


def solution(mesh):
    in_specs = (
        P(None, ("kv", "tp")),
        P("kv"),
        P("kv", "tp"),
        P("kv", "tp"),
        P("kv", "tp"),
        P("kv", "tp"),
        P("tp"),
        P("kv", "tp", None, None),
        P(),
        P("tp", "kv"),
        P("kv"),
        P("kv", "tp"),
        P("kv", "tp"),
        P("tp", "kv"),
    )
    out_specs = (P(None, ("kv", "tp")), P("kv", "tp", None, None))
    body = functools.partial(pick_body, n_kv=mesh.shape["kv"], n_tp=mesh.shape["tp"])
    return jax.shard_map(body, mesh=mesh, in_specs=in_specs, out_specs=out_specs, check_vma=False)
```
